256 devices in a mesh: grp: 4 (over y, x), ep: 64 (over z, core).
Axes of the slice: x: 2, y: 2, z: 32, core: 2. Of those that a mesh axis runs over, the one named last changes fastest.
The devices are a block of a 4x8x32 slice.
Arguments:
- tokens: bfloat16 [65536, 2048], P(('grp', 'ep')), parts along dimension 0, may hold values from -6 to 6
- norm_gain: float32 [2048], replicated, may hold values from 0.1 to 1.9
- route_ids: int32 [65536, 2], P(('grp', 'ep')), parts along dimension 0, may hold values from 0 to 63, as said below
- route_slots: int32 [65536, 2], P(('grp', 'ep')), parts along dimension 0, may hold values from 0 to 11, as said below
- route_weights: float32 [65536, 2], P(('grp', 'ep')), parts along dimension 0, may hold values from 0.1 to 1
- w_gate: bfloat16 [64, 2048, 512], P('ep'), may hold values from -0.125 to 0.125
- w_up: bfloat16 [64, 2048, 512], P('ep'), may hold values from -0.125 to 0.125
- w_down: bfloat16 [64, 512, 2048], P('ep'), may hold values from -0.25 to 0.25
Outputs:
- expert_mix: bfloat16 [65536, 2048], P(('grp', 'ep')), parts along dimension 0
The draws below stay inside these ranges and needn't reach their ends.
There are 4 independent parts, one for each index of `grp`. The reference program is written for one: setup_inputs(seed, part) draws one part's arguments, and reference() takes and returns one part's arrays. A program takes and returns all parts, laid end to end along the dimension named above; an argument that names none is the same for every part. Nothing has to cross between parts.
Inputs may be any that keep to these rules, and one draw needn't show every extreme that they name: `route_ids`: expert e belongs to group e // 16. Each token names 2 different experts of one group. In each aligned block of 256 tokens (the rows of one device) no expert is named more than 12 times, and some expert exactly 12 times. `route_slots`: in each aligned block of 256 tokens, the entries that name one expert hold distinct slots 0, 1, ... up to their count less one.
All inputs are finite; a program needn't handle non-finite values.
Results may differ from the reference program's by a relative error of at most 0.007.
Values may be sent and summed in bfloat16 or wider, within the bound.
A program may use at most 64 MiB of HBM per device.

```python
import math
import jax
import jax.numpy as jnp
from jax import lax

D = 2048
FE = 512
TOPK = 2
TOK_DEV = 256
EXPERTS = 64
CAP = 12
TOKENS = 16384


def route_table(key):
    n_blocks = TOKENS // TOK_DEV
    per_group = EXPERTS // 4
    busy_count = CAP * per_group // 2
    rest_count = TOK_DEV - busy_count
    block_keys = jax.random.split(jax.random.fold_in(key, 7), n_blocks)

    def one_block(block_key):
        key_busy, key_first, key_second, key_perm, key_base, key_shift = jax.random.split(block_key, 6)
        busy = jax.random.randint(key_busy, (), 0, 4)
        low_first = jnp.maximum(0, rest_count - 2 * busy_count)
        high_first = jnp.minimum(busy_count, rest_count)
        count_first = jax.random.randint(key_first, (), low_first, high_first + 1)
        low_second = jnp.maximum(0, rest_count - count_first - busy_count)
        high_second = jnp.minimum(busy_count, rest_count - count_first)
        count_second = jax.random.randint(key_second, (), low_second, high_second + 1)
        others = jnp.stack([count_first, count_second, rest_count - count_first - count_second]).astype(jnp.int32)
        group_ids = jnp.arange(4, dtype=jnp.int32)
        other_idx = jnp.clip(group_ids - (group_ids > busy).astype(jnp.int32), 0, 2)
        counts = jnp.where(group_ids == busy, busy_count, others[other_idx]).astype(jnp.int32)
        ends = jnp.cumsum(counts)
        starts = ends - counts
        places = jnp.arange(TOK_DEV, dtype=jnp.int32)
        group_sorted = jnp.sum((places[:, None] >= ends[None, :3]).astype(jnp.int32), axis=1)
        rank_sorted = places - starts[group_sorted]
        perm = jax.random.permutation(key_perm, TOK_DEV)
        group_tok = jnp.zeros((TOK_DEV,), jnp.int32).at[perm].set(group_sorted)
        rank_tok = jnp.zeros((TOK_DEV,), jnp.int32).at[perm].set(rank_sorted)
        base = jax.random.randint(key_base, (4,), 0, per_group)
        shift = jax.random.randint(key_shift, (4,), 1, per_group)
        first = group_tok * per_group + (base[group_tok] + rank_tok) % per_group
        second = group_tok * per_group + (base[group_tok] + rank_tok + shift[group_tok]) % per_group
        ids = jnp.stack([first, second], axis=1).astype(jnp.int32)
        flat_ids = ids.reshape(-1)
        onehot = (flat_ids[:, None] == jnp.arange(EXPERTS, dtype=jnp.int32)[None, :]).astype(jnp.int32)
        slots = jnp.sum(jnp.cumsum(onehot, axis=0) * onehot, axis=1) - 1
        return (ids, slots.reshape(TOK_DEV, 2).astype(jnp.int32))
    ids, slots = jax.vmap(one_block)(block_keys)
    return (ids.reshape(TOKENS, 2), slots.reshape(TOKENS, 2))


def draw_route_ids(key, part):
    return route_table(key)[0]


def draw_route_slots(key, part):
    return route_table(key)[1]


def block_levels(rng, extent, shards, low, largest):
    loudness, own = 1.0, jax.random.fold_in(rng, 6)
    for dim, shards_of in shards:
        heights = jnp.exp(jax.random.uniform(jax.random.fold_in(own, dim), (shards_of,), jnp.float32, low / len(shards), largest / len(shards)))
        loudness = loudness * jnp.repeat(heights, extent[dim] // shards_of).reshape([-1 if axis == dim else 1 for axis in range(len(extent))])
    return loudness


def scatter_about(key, dims, spread, reach, cuts=(), kind=jnp.bfloat16):
    drawn = spread * jax.random.normal(key, dims, jnp.float32)
    if cuts:
        drawn = drawn * block_levels(key, dims, cuts, -0.22, 0.18)
    return jnp.clip(drawn, -reach, reach).astype(kind)


def setup_inputs(seed: int = 0, part: int = 0) -> dict:
    streams_of = jax.random.split(jax.random.key(seed), 9)
    own_keys = jax.random.split(jax.random.fold_in(streams_of[8], part), 9)
    return {
        "tokens": scatter_about(own_keys[0], (TOKENS, D), 1.0, 6.0, ((0, 64),)),
        "norm_gain": jnp.clip(1.0 + 0.18 * jax.random.normal(streams_of[1], (D,), jnp.float32), 0.1, 1.9),
        "route_ids": draw_route_ids(jax.random.fold_in(jax.random.fold_in(streams_of[8], part), 71), part),
        "route_slots": draw_route_slots(jax.random.fold_in(jax.random.fold_in(streams_of[8], part), 71), part),
        "route_weights": jnp.clip(jnp.exp(math.log(1.0) - 2.3025851 * jax.random.uniform(own_keys[4], (TOKENS, TOPK), jnp.float32) ** block_levels(own_keys[4], (TOKENS, TOPK), ((0, 64),), -0.2, 0.2)), 0.1, 1.0),
        "w_gate": scatter_about(streams_of[5], (EXPERTS, D, FE), D ** -0.5, 0.125, ((0, 64),)),
        "w_up": scatter_about(streams_of[6], (EXPERTS, D, FE), D ** -0.5, 0.125, ((0, 64),)),
        "w_down": scatter_about(streams_of[7], (EXPERTS, FE, D), FE ** -0.5, 0.25, ((0, 64),)),
    }


def reference(tokens, norm_gain, route_ids, route_slots, route_weights, w_gate, w_up, w_down):
    tok_f32 = tokens.astype(jnp.float32)
    scale = lax.rsqrt(lax.optimization_barrier(jnp.mean(tok_f32 * tok_f32, axis=-1, keepdims=True)) + 1e-06)
    normed = (tok_f32 * scale * norm_gain.astype(jnp.float32)).astype(jnp.bfloat16)
    n_blocks = TOKENS // TOK_DEV
    block_of = (jnp.arange(TOKENS, dtype=jnp.int32) // TOK_DEV).astype(jnp.int32)
    place_idx = (route_ids * (n_blocks * CAP) + block_of[:, None] * CAP + route_slots).astype(jnp.int32)
    buffer = jnp.zeros((EXPERTS * n_blocks * CAP, D), jnp.bfloat16)
    buffer = buffer.at[place_idx.reshape(-1)].set(jnp.repeat(normed, TOPK, axis=0))
    buffer = buffer.reshape(EXPERTS, n_blocks * CAP, D)

    def expert_apply(args):
        rows_in, gate_w, up_w, down_w = args
        gate_act = jnp.dot(rows_in, gate_w, preferred_element_type=jnp.float32)
        up_act = jnp.dot(rows_in, up_w, preferred_element_type=jnp.float32)
        hidden = (jax.nn.silu(gate_act) * up_act).astype(jnp.bfloat16)
        return jnp.dot(hidden, down_w, preferred_element_type=jnp.float32).astype(jnp.bfloat16)
    results = lax.map(expert_apply, (buffer, w_gate, w_up, w_down))
    flat_rows = results.reshape(EXPERTS * n_blocks * CAP, D)
    picked = flat_rows[place_idx].astype(jnp.float32)
    mixed = lax.optimization_barrier(jnp.sum(route_weights[:, :, None] * picked, axis=1))
    return mixed.astype(jnp.bfloat16)
```

```python
import functools

import jax
import jax.numpy as jnp
from jax import lax
from jax.experimental import pallas as pl
from jax.experimental.pallas import tpu as pltpu
from jax.sharding import PartitionSpec as P

MESH = pl.DeviceIdType.MESH
GROUP = 16
HALF = GROUP // 2
CUTS = 4
F32 = jnp.float32
BF16 = jnp.bfloat16


def onehot(mask):
    return jnp.where(mask, 1.0, 0.0).astype(BF16)


def iota(shape, dim):
    return lax.broadcasted_iota(jnp.int32, shape, dim).astype(F32)


def exact_dot_nt(a, b):
    return lax.dot_general(
        a, b, (((1,), (1,)), ((), ())), precision=lax.Precision.HIGHEST, preferred_element_type=F32
    )


def dot(a, b):
    return jnp.dot(a, b, preferred_element_type=F32)


def kernel(
    n, cap, bundle, tab_ref, tok_ref, gain_ref, wg_hbm, wu_hbm, wd_hbm, out_ref,
    wg, wu, wd, nrm, pick, bout, bin_, mout, min_, xs, xin, zs, zin, rs, rin, xstk, ystk, perm, place,
    wsem, bsend, brecv, msend, mrecv, xsend, xrecv, zsend, zrecv, rsend, rrecv,
):
    toks, feats = tok_ref.shape
    piece = feats // CUTS
    unit = CUTS * cap
    rows = GROUP * unit
    quad = 4 * unit
    slots = 4
    me = lax.axis_index("ep")
    base = (me // GROUP) * GROUP
    r = me % GROUP
    upper = (r // HALF)
    sign = 2 * upper - 1

    def wrap(dev):
        return (dev + 4 * n) % n

    def target(k):
        return wrap(me + sign * (2 * (k % 2) - 1) * HALF * k)

    def source(k):
        return wrap(me + sign * HALF * k)

    copies = [
        pltpu.make_async_copy(src, dst, wsem.at[i])
        for i, (src, dst) in enumerate(((wg_hbm.at[0], wg), (wu_hbm.at[0], wu), (wd_hbm.at[0], wd)))
    ]
    for c in copies:
        c.start()

    barrier = pltpu.get_barrier_semaphore()

    def greet(i, _):
        pl.semaphore_signal(barrier, inc=1, device_id={"ep": base + (r + i) % GROUP}, device_id_type=MESH)
        return 0

    bin_[:, :, bundle:, :] = jnp.zeros_like(bin_[:, :, bundle:, :])
    for k in range(slots):
        lo = k * 128 + bundle
        rin[:, lo : lo + 128 - bundle, :] = jnp.zeros((CUTS, 128 - bundle, piece), BF16)

    lax.fori_loop(1, GROUP, greet, 0)
    for other in (wrap(me + HALF * sign), wrap(me + 3 * HALF * sign), wrap(me + 2 * HALF), wrap(me - 2 * HALF)):
        pl.semaphore_signal(barrier, inc=1, device_id={"ep": other}, device_id_type=MESH)

    step = 32
    gain = gain_ref[...]

    def norm(i, _):
        at = pl.ds(pl.multiple_of(i * step, step), step)
        x = tok_ref[at, :].astype(F32)
        scale = lax.rsqrt(jnp.mean(x * x, axis=-1, keepdims=True) + 1e-06)
        nrm[at, :] = (x * scale * gain).astype(BF16)
        return 0

    lax.fori_loop(0, toks // step, norm, 0)

    tab = tab_ref[...]
    slot_row = tab[0:1, :]
    of_slot = onehot(iota((8, toks), 0) == slot_row)
    before = onehot(iota((toks, toks), 0) < iota((toks, toks), 1))
    ranks = dot(of_slot, before)
    rank_row = jnp.sum(of_slot.astype(F32) * ranks, axis=0, keepdims=True)
    key_row = slot_row * 128.0 + rank_row
    mask = iota((slots * 128, toks), 0) == key_row
    pick[...] = onehot(mask)
    meta = exact_dot_nt(tab, jnp.where(mask, 1.0, 0.0).astype(F32))
    for k in range(slots):
        mout[k] = meta[:, k * 128 : (k + 1) * 128]
    eye = jnp.where(iota((toks, toks), 0) == iota((toks, toks), 1), 1.0, 0.0).astype(F32)
    key_col = exact_dot_nt(eye, jnp.broadcast_to(key_row, (8, toks)))[:, 0:1]
    place[...] = onehot(iota((toks, slots * 128), 1) == key_col)

    for c in range(CUTS):
        bout[c] = dot(pick[...], nrm[:, c * piece : (c + 1) * piece]).astype(BF16)

    i0 = iota((quad, quad), 0)
    a0 = jnp.floor((i0 + 0.5) / unit)
    b0 = jnp.floor((i0 - a0 * unit + 0.5) / cap)
    swapped = b0 * unit + a0 * cap + (i0 - a0 * unit - b0 * cap)
    perm[...] = onehot(iota((quad, quad), 1) == swapped)

    pl.semaphore_wait(barrier, GROUP - 1 + 4)

    def send_bundle(k):
        pltpu.make_async_remote_copy(
            src_ref=mout.at[k], dst_ref=min_.at[k], send_sem=msend.at[k], recv_sem=mrecv.at[k],
            device_id={"ep": target(k)}, device_id_type=MESH,
        ).start()
        pltpu.make_async_remote_copy(
            src_ref=bout.at[:, pl.ds(k * 128, bundle)], dst_ref=bin_.at[k, :, pl.ds(0, bundle)],
            send_sem=bsend.at[k], recv_sem=brecv.at[k],
            device_id={"ep": target(k)}, device_id_type=MESH,
        ).start()

    own_meta = pltpu.make_async_copy(mout.at[0], min_.at[0], mrecv.at[0])
    own_rows = pltpu.make_async_copy(bout.at[:, pl.ds(0, bundle)], bin_.at[0, :, pl.ds(0, bundle)], brecv.at[0])
    own_meta.start()
    own_rows.start()
    for k in range(1, slots):
        send_bundle(k)

    def spread(src, dst, k, send_sem, recv_sem):
        mine = pl.ds(pl.multiple_of(r * unit, 16), unit)

        def one(i, _):
            other = (r + i) % GROUP
            pltpu.make_async_remote_copy(
                src_ref=src.at[k, pl.ds(pl.multiple_of(other * unit, 16), unit)], dst_ref=dst.at[k, mine],
                send_sem=send_sem.at[k], recv_sem=recv_sem.at[k],
                device_id={"ep": base + other}, device_id_type=MESH,
            ).start()
            return 0

        lax.fori_loop(1, GROUP, one, 0)
        pltpu.make_async_copy(src.at[k, mine], dst.at[k, mine], recv_sem.at[k]).start()

    def landed(ref, sem):
        pltpu.make_async_copy(ref, ref, sem).wait()

    def gather(k):
        landed(min_.at[k], mrecv.at[k])
        landed(bin_.at[k, :, pl.ds(0, bundle)], brecv.at[k])
        m = min_[k]
        both = []
        for i in (1, 2):
            j = jnp.where(m[i : i + 1] > 0.0, m[i : i + 1] - 1.0, -1000.0)
            both.append(jnp.concatenate([j + float(cap * c) for c in range(CUTS)], axis=1))

        def part(b, _):
            at = pl.ds(pl.multiple_of(b * quad, quad), quad)
            row = iota((quad, CUTS * 128), 0) + (b * quad).astype(F32)
            sel = onehot((row == both[0]) | (row == both[1]))
            xs[k, at, :] = dot(sel, bin_[k].reshape(CUTS * 128, piece)).astype(BF16)
            return 0

        lax.fori_loop(0, 4, part, 0)
        spread(xs, xin, k, xsend, xrecv)

    def expert(k):
        landed(xin.at[k], xrecv.at[k])
        for b in range(4):
            y = dot(perm[...], xin[k, b * quad : (b + 1) * quad, :]).astype(BF16)
            for c in range(CUTS):
                xstk[b * unit : (b + 1) * unit, c * piece : (c + 1) * piece] = y[c * unit : (c + 1) * unit]
        gate = dot(xstk[...], wg[...])
        up = dot(xstk[...], wu[...])
        hidden = (gate / (1.0 + jnp.exp(-gate)) * up).astype(BF16)
        for c in range(CUTS):
            y = dot(hidden, wd[:, c * piece : (c + 1) * piece]).astype(BF16)
            for b in range(4):
                ystk[b, c * unit : (c + 1) * unit, :] = y[b * unit : (b + 1) * unit]
        for b in range(4):
            zs[k, b * quad : (b + 1) * quad, :] = dot(perm[...], ystk[b]).astype(BF16)
        spread(zs, zin, k, zsend, zrecv)

    def combine(k):
        landed(zin.at[k], zrecv.at[k])
        eye = jnp.where(iota((128, 128), 0) == iota((128, 128), 1), 1.0, 0.0).astype(F32)
        cols = exact_dot_nt(eye, min_[k])
        j1 = jnp.where(cols[:, 1:2] > 0.0, cols[:, 1:2] - 1.0, -1000.0)
        j2 = jnp.where(cols[:, 2:3] > 0.0, cols[:, 2:3] - 1.0, -1000.0)
        w1, w2 = cols[:, 3:4], cols[:, 4:5]
        lane = iota((128, rows), 1)
        for c in range(CUTS):
            y1 = dot(onehot(lane == j1 + float(cap * c)), zin[k])
            y2 = dot(onehot(lane == j2 + float(cap * c)), zin[k])
            rs[k, c] = (w1 * y1 + w2 * y2).astype(BF16)
        dst = rin.at[:, pl.ds(pl.multiple_of(k * 128, 128), bundle)]

        @pl.when(k == 0)
        def _():
            pltpu.make_async_copy(rs.at[0, :, pl.ds(0, bundle)], dst, rrecv.at[0]).start()

        @pl.when(k > 0)
        def _():
            pltpu.make_async_remote_copy(
                src_ref=rs.at[k, :, pl.ds(0, bundle)], dst_ref=dst, send_sem=rsend.at[k], recv_sem=rrecv.at[k],
                device_id={"ep": source(k)}, device_id_type=MESH,
            ).start()

    def stage(t, _):
        @pl.when(t < slots)
        def _():
            gather(t)

        @pl.when(t == 1)
        def _():
            for c in copies:
                c.wait()

        @pl.when((t >= 1) & (t < slots + 1))
        def _():
            expert(t - 1)

        @pl.when(t >= 2)
        def _():
            combine(t - 2)

        return 0

    lax.fori_loop(0, slots + 2, stage, 0)

    for k in range(slots):
        landed(rin.at[:, pl.ds(k * 128, bundle)], rrecv.at[k])
    for c in range(CUTS):
        out_ref[:, c * piece : (c + 1) * piece] = dot(place[...], rin[c]).astype(BF16)

    for k in range(slots):
        for buf, sem in ((xs, xsend), (zs, zsend)):
            landed(buf.at[k, pl.ds(0, rows - unit)], sem.at[k])
    for k in range(1, slots):
        landed(mout.at[k], msend.at[k])
        landed(bout.at[:, pl.ds(k * 128, bundle)], bsend.at[k])
        landed(rs.at[k, :, pl.ds(0, bundle)], rsend.at[k])


def shards(n, tokens, norm_gain, route_ids, route_slots, route_weights, w_gate, w_up, w_down):
    toks, feats = tokens.shape
    hidden = w_gate.shape[2]
    top = route_ids.shape[1]
    cap = 3 * top * toks // (2 * n)
    bundle = GROUP * cap // top
    piece = feats // CUTS
    unit = CUTS * cap
    rows = GROUP * unit
    slots = 4

    me = lax.axis_index("ep")
    rel = (route_ids[:, 0] // GROUP - me // GROUP + slots) % slots
    lower = (me % GROUP) < HALF
    first = jnp.where(lower, 3, 1)
    slot = jnp.where(rel == 0, 0, jnp.where(rel == 2, 3, jnp.where(rel == first, 1, 2)))
    spots = (route_ids % GROUP) * unit + route_slots + 1
    zero = jnp.zeros((toks,), F32)
    tab = jnp.stack(
        [slot.astype(F32), spots[:, 0].astype(F32), spots[:, 1].astype(F32), route_weights[:, 0], route_weights[:, 1],
         zero, zero, zero]
    )
    vmem = pl.BlockSpec(memory_space=pltpu.VMEM)
    hbm = pl.BlockSpec(memory_space=pl.ANY)
    return pl.pallas_call(
        functools.partial(kernel, n, cap, bundle),
        out_shape=jax.ShapeDtypeStruct((toks, feats), BF16),
        in_specs=[vmem, vmem, vmem, hbm, hbm, hbm],
        out_specs=vmem,
        scratch_shapes=[
            pltpu.VMEM((feats, hidden), BF16),
            pltpu.VMEM((feats, hidden), BF16),
            pltpu.VMEM((hidden, feats), BF16),
            pltpu.VMEM((toks, feats), BF16),
            pltpu.VMEM((slots * 128, toks), BF16),
            pltpu.VMEM((CUTS, slots * 128, piece), BF16),
            pltpu.VMEM((slots, CUTS, 128, piece), BF16),
            pltpu.VMEM((slots, 8, 128), F32),
            pltpu.VMEM((slots, 8, 128), F32),
            pltpu.VMEM((slots, rows, piece), BF16),
            pltpu.VMEM((slots, rows, piece), BF16),
            pltpu.VMEM((slots, rows, piece), BF16),
            pltpu.VMEM((slots, rows, piece), BF16),
            pltpu.VMEM((slots, CUTS, 128, piece), BF16),
            pltpu.VMEM((CUTS, slots * 128, piece), BF16),
            pltpu.VMEM((GROUP * cap, feats), BF16),
            pltpu.VMEM((4, 4 * unit, piece), BF16),
            pltpu.VMEM((4 * unit, 4 * unit), BF16),
            pltpu.VMEM((toks, slots * 128), BF16),
            pltpu.SemaphoreType.DMA((3,)),
        ] + [pltpu.SemaphoreType.DMA((slots,))] * 10,
        compiler_params=pltpu.CompilerParams(
            collective_id=0, has_side_effects=True, vmem_limit_bytes=60 * 1024 * 1024
        ),
    )(tab, tokens, norm_gain.reshape(1, feats), w_gate, w_up, w_down)


def solution(mesh):
    both = ("grp", "ep")
    in_specs = (
        P(both, None), P(None), P(both, None), P(both, None), P(both, None),
        P("ep", None, None), P("ep", None, None), P("ep", None, None),
    )
    return jax.shard_map(
        functools.partial(shards, mesh.shape["ep"]), mesh=mesh, in_specs=in_specs, out_specs=P(both, None),
        check_vma=False,
    )
```

```python
import functools

import jax
import jax.numpy as jnp
from jax import lax
from jax.experimental import pallas as pl
from jax.experimental.pallas import tpu as pltpu
from jax.sharding import PartitionSpec as P

MESH = pl.DeviceIdType.MESH
GROUP = 16
HALF = GROUP // 2
CUTS = 4
SENDS = (3, 2, 1)
ET, CT = 2, 3

F32 = jnp.float32
BF16 = jnp.bfloat16


def far_order(one, r):
    lax.fori_loop(0, GROUP - 1 - r, lambda i, a: one(GROUP - 1 - i, a), 0)
    lax.fori_loop(0, r, one, 0)


def onehot(mask):
    return jnp.where(mask, 1.0, 0.0).astype(BF16)


def iota(shape, dim):
    return lax.broadcasted_iota(jnp.int32, shape, dim).astype(F32)


def exact_dot_nt(a, b):
    return lax.dot_general(
        a, b, (((1,), (1,)), ((), ())), precision=lax.Precision.HIGHEST, preferred_element_type=F32
    )


def dot(a, b):
    return jnp.dot(a, b, preferred_element_type=F32)


def kernel(
    n, cap, bundle, ids_ref, spots_ref, mix_ref, tok_hbm, gain_ref, wg_hbm, wu_hbm, wd_hbm, out_ref,
    tok_ref, wg, wu, wd, nrm, pick, bout, bin_, mout, min_, xs, xin, zs, zin, rs, rin, xstk, ystk, perm, place,
    tsem, wsem, bsend, brecv, msend, mrecv, xsend, xrecv, zsend, zrecv, rsend, rrecv,
):
    toks, feats = tok_hbm.shape
    piece = feats // CUTS
    unit = CUTS * cap
    rows = GROUP * unit
    quad = 4 * unit
    slots = 4
    me = lax.axis_index("ep")
    base = (me // GROUP) * GROUP
    r = me % GROUP
    upper = (r // HALF)
    sign = 2 * upper - 1

    def wrap(dev):
        return (dev + 4 * n) % n

    def target(k):
        return wrap(me + sign * (2 * (k % 2) - 1) * HALF * k)

    def source(k):
        return wrap(me + sign * HALF * k)

    barrier = pltpu.get_barrier_semaphore()

    def greet(i, _):
        pl.semaphore_signal(barrier, inc=1, device_id={"ep": base + (r + i) % GROUP}, device_id_type=MESH)
        return 0

    lax.fori_loop(1, GROUP, greet, 0)
    for other in (wrap(me + HALF * sign), wrap(me + 3 * HALF * sign), wrap(me + 2 * HALF), wrap(me - 2 * HALF)):
        pl.semaphore_signal(barrier, inc=1, device_id={"ep": other}, device_id_type=MESH)

    tokens_in = pltpu.make_async_copy(tok_hbm, tok_ref, tsem)
    tokens_in.start()
    copies = [
        pltpu.make_async_copy(src, dst, wsem.at[i])
        for i, (src, dst) in enumerate(((wg_hbm.at[0], wg), (wu_hbm.at[0], wu), (wd_hbm.at[0], wd)))
    ]
    for c in copies:
        c.start()

    bin_[:, :, bundle:, :] = jnp.zeros_like(bin_[:, :, bundle:, :])
    for k in range(slots):
        lo = k * 128 + bundle
        rin[:, lo : lo + 128 - bundle, :] = jnp.zeros((CUTS, 128 - bundle, piece), BF16)

    step = 32
    gain = gain_ref[...]

    def norm(i, _):
        at = pl.ds(pl.multiple_of(i * step, step), step)
        x = tok_ref[at, :].astype(F32)
        scale = lax.rsqrt(jnp.mean(x * x, axis=-1, keepdims=True) + 1e-06)
        nrm[at, :] = (x * scale * gain).astype(BF16)
        return 0

    tokens_in.wait()
    lax.fori_loop(0, toks // step, norm, 0)

    ids = ids_ref[...]
    team = ids // GROUP
    rel = (team[0:1, :] - me // GROUP + slots) % slots
    near = 3 - 2 * upper
    slot_row = jnp.where(rel == 0, 0, jnp.where(rel == 2, 3, jnp.where(rel == near, 1, 2))).astype(F32)
    spots = ((ids - team * GROUP) * unit + spots_ref[...] + 1).astype(F32)
    tab = jnp.concatenate([slot_row, spots, mix_ref[...], jnp.zeros((3, toks), F32)], axis=0)
    of_slot = onehot(iota((8, toks), 0) == slot_row)
    before = onehot(iota((toks, toks), 0) < iota((toks, toks), 1))
    ranks = dot(of_slot, before)
    rank_row = jnp.sum(of_slot.astype(F32) * ranks, axis=0, keepdims=True)
    key_row = slot_row * 128.0 + rank_row
    mask = iota((slots * 128, toks), 0) == key_row
    pick[...] = onehot(mask)
    meta = exact_dot_nt(tab, jnp.where(mask, 1.0, 0.0).astype(F32))
    for k in range(slots):
        mout[k] = meta[:, k * 128 : (k + 1) * 128]
    eye = jnp.where(iota((toks, toks), 0) == iota((toks, toks), 1), 1.0, 0.0).astype(F32)
    key_col = exact_dot_nt(eye, jnp.broadcast_to(key_row, (8, toks)))[:, 0:1]
    place[...] = onehot(iota((toks, slots * 128), 1) == key_col)

    for c in range(CUTS):
        bout[c] = dot(pick[...], nrm[:, c * piece : (c + 1) * piece]).astype(BF16)

    i0 = iota((quad, quad), 0)
    a0 = jnp.floor((i0 + 0.5) / unit)
    b0 = jnp.floor((i0 - a0 * unit + 0.5) / cap)
    swapped = b0 * unit + a0 * cap + (i0 - a0 * unit - b0 * cap)
    perm[...] = onehot(iota((quad, quad), 1) == swapped)

    pl.semaphore_wait(barrier, GROUP - 1 + 4)

    def send_bundle(k):
        pltpu.make_async_remote_copy(
            src_ref=mout.at[k], dst_ref=min_.at[k], send_sem=msend.at[k], recv_sem=mrecv.at[k],
            device_id={"ep": target(k)}, device_id_type=MESH,
        ).start()
        pltpu.make_async_remote_copy(
            src_ref=bout.at[:, pl.ds(k * 128, bundle)], dst_ref=bin_.at[k, :, pl.ds(0, bundle)],
            send_sem=bsend.at[k], recv_sem=brecv.at[k],
            device_id={"ep": target(k)}, device_id_type=MESH,
        ).start()

    own_meta = pltpu.make_async_copy(mout.at[0], min_.at[0], mrecv.at[0])
    own_rows = pltpu.make_async_copy(bout.at[:, pl.ds(0, bundle)], bin_.at[0, :, pl.ds(0, bundle)], brecv.at[0])
    own_meta.start()
    own_rows.start()
    for k in SENDS:
        send_bundle(k)

    def spread(src, dst, k, send_sem, recv_sem):
        mine = pl.ds(pl.multiple_of(r * unit, 16), unit)

        def one(i, _):
            other = i
            pltpu.make_async_remote_copy(
                src_ref=src.at[k, pl.ds(pl.multiple_of(other * unit, 16), unit)], dst_ref=dst.at[k, mine],
                send_sem=send_sem.at[k], recv_sem=recv_sem.at[k],
                device_id={"ep": base + other}, device_id_type=MESH,
            ).start()
            return 0

        far_order(one, r)
        pltpu.make_async_copy(src.at[k, mine], dst.at[k, mine], recv_sem.at[k]).start()

    def landed(ref, sem):
        pltpu.make_async_copy(ref, ref, sem).wait()

    def gather(k):
        landed(min_.at[k], mrecv.at[k])
        landed(bin_.at[k, :, pl.ds(0, bundle)], brecv.at[k])
        m = min_[k]
        both = []
        for i in (1, 2):
            j = jnp.where(m[i : i + 1] > 0.0, m[i : i + 1] - 1.0, -1000.0)
            both.append(jnp.concatenate([j + float(cap * c) for c in range(CUTS)], axis=1))

        def part(b, _):
            at = pl.ds(pl.multiple_of(b * quad, quad), quad)
            row = iota((quad, CUTS * 128), 0) + (b * quad).astype(F32)
            sel = onehot((row == both[0]) | (row == both[1]))
            xs[k, at, :] = dot(sel, bin_[k].reshape(CUTS * 128, piece)).astype(BF16)
            return 0

        lax.fori_loop(0, 4, part, 0)
        spread(xs, xin, k, xsend, xrecv)

    def expert(k):
        landed(xin.at[k], xrecv.at[k])
        for b in range(4):
            y = dot(perm[...], xin[k, b * quad : (b + 1) * quad, :]).astype(BF16)
            for c in range(CUTS):
                xstk[b * unit : (b + 1) * unit, c * piece : (c + 1) * piece] = y[c * unit : (c + 1) * unit]
        gate = dot(xstk[...], wg[...])
        up = dot(xstk[...], wu[...])
        hidden = (gate / (1.0 + jnp.exp(-gate)) * up).astype(BF16)
        for c in range(CUTS):
            y = dot(hidden, wd[:, c * piece : (c + 1) * piece]).astype(BF16)
            for b in range(4):
                ystk[b, c * unit : (c + 1) * unit, :] = y[b * unit : (b + 1) * unit]
        for b in range(4):
            zs[k, b * quad : (b + 1) * quad, :] = dot(perm[...], ystk[b]).astype(BF16)
        spread(zs, zin, k, zsend, zrecv)

    def combine(k):
        landed(zin.at[k], zrecv.at[k])
        eye = jnp.where(iota((128, 128), 0) == iota((128, 128), 1), 1.0, 0.0).astype(F32)
        cols = exact_dot_nt(eye, min_[k])
        j1 = jnp.where(cols[:, 1:2] > 0.0, cols[:, 1:2] - 1.0, -1000.0)
        j2 = jnp.where(cols[:, 2:3] > 0.0, cols[:, 2:3] - 1.0, -1000.0)
        w1, w2 = cols[:, 3:4], cols[:, 4:5]
        lane = iota((128, rows), 1)
        for c in range(CUTS):
            y1 = dot(onehot(lane == j1 + float(cap * c)), zin[k])
            y2 = dot(onehot(lane == j2 + float(cap * c)), zin[k])
            rs[k, c] = (w1 * y1 + w2 * y2).astype(BF16)
        dst = rin.at[:, pl.ds(pl.multiple_of(k * 128, 128), bundle)]

        @pl.when(k == 0)
        def _():
            pltpu.make_async_copy(rs.at[0, :, pl.ds(0, bundle)], dst, rrecv.at[0]).start()

        @pl.when(k > 0)
        def _():
            pltpu.make_async_remote_copy(
                src_ref=rs.at[k, :, pl.ds(0, bundle)], dst_ref=dst, send_sem=rsend.at[k], recv_sem=rrecv.at[k],
                device_id={"ep": source(k)}, device_id_type=MESH,
            ).start()

    def stage(t, _):
        @pl.when(t < 4)
        def _():
            gather((slots - t) % slots)

        @pl.when(t == 1)
        def _():
            for c in copies:
                c.wait()

        @pl.when((t >= ET) & (t < ET + slots))
        def _():
            expert(ET + slots - 1 - t)

        @pl.when((t >= CT) & (t < CT + slots))
        def _():
            combine(CT + slots - 1 - t)

        return 0

    lax.fori_loop(0, CT + slots, stage, 0)

    for k in range(slots):
        landed(rin.at[:, pl.ds(k * 128, bundle)], rrecv.at[k])
    for c in range(CUTS):
        out_ref[:, c * piece : (c + 1) * piece] = dot(place[...], rin[c]).astype(BF16)

    for k in range(slots):
        for buf, sem in ((xs, xsend), (zs, zsend)):
            landed(buf.at[k, pl.ds(0, rows - unit)], sem.at[k])
    for k in range(1, slots):
        landed(mout.at[k], msend.at[k])
        landed(bout.at[:, pl.ds(k * 128, bundle)], bsend.at[k])
        landed(rs.at[k, :, pl.ds(0, bundle)], rsend.at[k])


def shards(n, tokens, norm_gain, route_ids, route_slots, route_weights, w_gate, w_up, w_down):
    toks, feats = tokens.shape
    hidden = w_gate.shape[2]
    top = route_ids.shape[1]
    cap = 3 * top * toks // (2 * n)
    bundle = GROUP * cap // top
    piece = feats // CUTS
    unit = CUTS * cap
    rows = GROUP * unit
    slots = 4

    vmem = pl.BlockSpec(memory_space=pltpu.VMEM)
    hbm = pl.BlockSpec(memory_space=pl.ANY)
    return pl.pallas_call(
        functools.partial(kernel, n, cap, bundle),
        out_shape=jax.ShapeDtypeStruct((toks, feats), BF16),
        in_specs=[vmem, vmem, vmem, hbm, vmem, hbm, hbm, hbm],
        out_specs=vmem,
        scratch_shapes=[
            pltpu.VMEM((toks, feats), BF16),
            pltpu.VMEM((feats, hidden), BF16),
            pltpu.VMEM((feats, hidden), BF16),
            pltpu.VMEM((hidden, feats), BF16),
            pltpu.VMEM((toks, feats), BF16),
            pltpu.VMEM((slots * 128, toks), BF16),
            pltpu.VMEM((CUTS, slots * 128, piece), BF16),
            pltpu.VMEM((slots, CUTS, 128, piece), BF16),
            pltpu.VMEM((slots, 8, 128), F32),
            pltpu.VMEM((slots, 8, 128), F32),
            pltpu.VMEM((slots, rows, piece), BF16),
            pltpu.VMEM((slots, rows, piece), BF16),
            pltpu.VMEM((slots, rows, piece), BF16),
            pltpu.VMEM((slots, rows, piece), BF16),
            pltpu.VMEM((slots, CUTS, 128, piece), BF16),
            pltpu.VMEM((CUTS, slots * 128, piece), BF16),
            pltpu.VMEM((GROUP * cap, feats), BF16),
            pltpu.VMEM((4, 4 * unit, piece), BF16),
            pltpu.VMEM((4 * unit, 4 * unit), BF16),
            pltpu.VMEM((toks, slots * 128), BF16),
            pltpu.SemaphoreType.DMA,
            pltpu.SemaphoreType.DMA((3,)),
        ] + [pltpu.SemaphoreType.DMA((slots,))] * 10,
        compiler_params=pltpu.CompilerParams(
            collective_id=0, has_side_effects=True, vmem_limit_bytes=60 * 1024 * 1024
        ),
    )(route_ids.T, route_slots.T, route_weights.T, tokens, norm_gain.reshape(1, feats), w_gate, w_up, w_down)


def solution(mesh):
    both = ("grp", "ep")
    in_specs = (
        P(both, None), P(None), P(both, None), P(both, None), P(both, None),
        P("ep", None, None), P("ep", None, None), P("ep", None, None),
    )
    return jax.shard_map(
        functools.partial(shards, mesh.shape["ep"]), mesh=mesh, in_specs=in_specs, out_specs=P(both, None),
        check_vma=False,
    )
```

```python
import functools

import jax
import jax.numpy as jnp
from jax import lax
from jax.experimental import pallas as pl
from jax.experimental.pallas import tpu as pltpu
from jax.sharding import PartitionSpec as P

MESH = pl.DeviceIdType.MESH
GROUP = 16
HALF = GROUP // 2
CUTS = 4
SENDS = (3, 2, 1)
ET, CT = 2, 4

F32 = jnp.float32
BF16 = jnp.bfloat16


def far_order(one, r):
    def pair(i, _):
        @pl.when(GROUP - 1 - i > r)
        def _():
            one(GROUP - 1 - i, 0)

        @pl.when(i < r)
        def _():
            one(i, 0)

        return 0

    lax.fori_loop(0, GROUP, pair, 0)


def onehot(mask):
    return jnp.where(mask, 1.0, 0.0).astype(BF16)


def iota(shape, dim):
    return lax.broadcasted_iota(jnp.int32, shape, dim).astype(F32)


def exact_dot_nt(a, b):
    return lax.dot_general(
        a, b, (((1,), (1,)), ((), ())), precision=lax.Precision.HIGHEST, preferred_element_type=F32
    )


def dot(a, b):
    return jnp.dot(a, b, preferred_element_type=F32)


def kernel(
    n, cap, bundle, ids_ref, spots_ref, mix_ref, tok_hbm, gain_ref, wg_hbm, wu_hbm, wd_hbm, out_ref,
    tok_ref, wg, wu, wd, nrm, pick, bout, bin_, mout, min_, xs, xin, zs, zin, rs, rin, xstk, ystk, perm, place,
    tsem, wsem, bsend, brecv, msend, mrecv, xsend, xrecv, zsend, zrecv, rsend, rrecv,
):
    toks, feats = tok_hbm.shape
    piece = feats // CUTS
    unit = CUTS * cap
    rows = GROUP * unit
    quad = 4 * unit
    slots = 4
    me = lax.axis_index("ep")
    base = (me // GROUP) * GROUP
    r = me % GROUP
    upper = (r // HALF)
    sign = 2 * upper - 1

    def wrap(dev):
        return (dev + 4 * n) % n

    def target(k):
        return wrap(me + sign * (2 * (k % 2) - 1) * HALF * k)

    def source(k):
        return wrap(me + sign * HALF * k)

    barrier = pltpu.get_barrier_semaphore()

    def greet(i, _):
        pl.semaphore_signal(barrier, inc=1, device_id={"ep": base + (r + i) % GROUP}, device_id_type=MESH)
        return 0

    lax.fori_loop(1, GROUP, greet, 0)
    for other in (wrap(me + HALF * sign), wrap(me + 3 * HALF * sign), wrap(me + 2 * HALF), wrap(me - 2 * HALF)):
        pl.semaphore_signal(barrier, inc=1, device_id={"ep": other}, device_id_type=MESH)

    tokens_in = pltpu.make_async_copy(tok_hbm, tok_ref, tsem)
    tokens_in.start()
    copies = [
        pltpu.make_async_copy(src, dst, wsem.at[i])
        for i, (src, dst) in enumerate(((wg_hbm.at[0], wg), (wu_hbm.at[0], wu), (wd_hbm.at[0], wd)))
    ]
    for c in copies:
        c.start()

    bin_[:, :, bundle:, :] = jnp.zeros_like(bin_[:, :, bundle:, :])
    for k in range(slots):
        lo = k * 128 + bundle
        rin[:, lo : lo + 128 - bundle, :] = jnp.zeros((CUTS, 128 - bundle, piece), BF16)

    step = 32
    gain = gain_ref[...]

    def norm(i, _):
        at = pl.ds(pl.multiple_of(i * step, step), step)
        x = tok_ref[at, :].astype(F32)
        scale = lax.rsqrt(jnp.mean(x * x, axis=-1, keepdims=True) + 1e-06)
        nrm[at, :] = (x * scale * gain).astype(BF16)
        return 0

    tokens_in.wait()
    lax.fori_loop(0, toks // step, norm, 0)

    ids = ids_ref[...]
    team = ids // GROUP
    rel = (team[0:1, :] - me // GROUP + slots) % slots
    near = 3 - 2 * upper
    slot_row = jnp.where(rel == 0, 0, jnp.where(rel == 2, 3, jnp.where(rel == near, 1, 2))).astype(F32)
    spots = ((ids - team * GROUP) * unit + spots_ref[...] + 1).astype(F32)
    tab = jnp.concatenate([slot_row, spots, mix_ref[...], jnp.zeros((3, toks), F32)], axis=0)
    of_slot = onehot(iota((8, toks), 0) == slot_row)
    before = onehot(iota((toks, toks), 0) < iota((toks, toks), 1))
    ranks = dot(of_slot, before)
    rank_row = jnp.sum(of_slot.astype(F32) * ranks, axis=0, keepdims=True)
    key_row = slot_row * 128.0 + rank_row
    mask = iota((slots * 128, toks), 0) == key_row
    pick[...] = onehot(mask)
    meta = exact_dot_nt(tab, jnp.where(mask, 1.0, 0.0).astype(F32))
    for k in range(slots):
        mout[k] = meta[:, k * 128 : (k + 1) * 128]
    eye = jnp.where(iota((toks, toks), 0) == iota((toks, toks), 1), 1.0, 0.0).astype(F32)
    key_col = exact_dot_nt(eye, jnp.broadcast_to(key_row, (8, toks)))[:, 0:1]
    place[...] = onehot(iota((toks, slots * 128), 1) == key_col)

    for c in range(CUTS):
        bout[c] = dot(pick[...], nrm[:, c * piece : (c + 1) * piece]).astype(BF16)

    i0 = iota((quad, quad), 0)
    a0 = jnp.floor((i0 + 0.5) / unit)
    b0 = jnp.floor((i0 - a0 * unit + 0.5) / cap)
    swapped = b0 * unit + a0 * cap + (i0 - a0 * unit - b0 * cap)
    perm[...] = onehot(iota((quad, quad), 1) == swapped)

    pl.semaphore_wait(barrier, GROUP - 1 + 4)

    def send_bundle(k):
        pltpu.make_async_remote_copy(
            src_ref=mout.at[k], dst_ref=min_.at[k], send_sem=msend.at[k], recv_sem=mrecv.at[k],
            device_id={"ep": target(k)}, device_id_type=MESH,
        ).start()
        pltpu.make_async_remote_copy(
            src_ref=bout.at[:, pl.ds(k * 128, bundle)], dst_ref=bin_.at[k, :, pl.ds(0, bundle)],
            send_sem=bsend.at[k], recv_sem=brecv.at[k],
            device_id={"ep": target(k)}, device_id_type=MESH,
        ).start()

    own_meta = pltpu.make_async_copy(mout.at[0], min_.at[0], mrecv.at[0])
    own_rows = pltpu.make_async_copy(bout.at[:, pl.ds(0, bundle)], bin_.at[0, :, pl.ds(0, bundle)], brecv.at[0])
    own_meta.start()
    own_rows.start()
    for k in SENDS:
        send_bundle(k)

    def spread(src, dst, k, send_sem, recv_sem):
        mine = pl.ds(pl.multiple_of(r * unit, 16), unit)

        def one(i, _):
            other = i
            pltpu.make_async_remote_copy(
                src_ref=src.at[k, pl.ds(pl.multiple_of(other * unit, 16), unit)], dst_ref=dst.at[k, mine],
                send_sem=send_sem.at[k], recv_sem=recv_sem.at[k],
                device_id={"ep": base + other}, device_id_type=MESH,
            ).start()
            return 0

        far_order(one, r)
        pltpu.make_async_copy(src.at[k, mine], dst.at[k, mine], recv_sem.at[k]).start()

    def landed(ref, sem):
        pltpu.make_async_copy(ref, ref, sem).wait()

    def gather(k):
        landed(min_.at[k], mrecv.at[k])
        landed(bin_.at[k, :, pl.ds(0, bundle)], brecv.at[k])
        m = min_[k]
        both = []
        for i in (1, 2):
            j = jnp.where(m[i : i + 1] > 0.0, m[i : i + 1] - 1.0, -1000.0)
            both.append(jnp.concatenate([j + float(cap * c) for c in range(CUTS)], axis=1))

        def part(b, _):
            at = pl.ds(pl.multiple_of(b * quad, quad), quad)
            row = iota((quad, CUTS * 128), 0) + (b * quad).astype(F32)
            sel = onehot((row == both[0]) | (row == both[1]))
            xs[k, at, :] = dot(sel, bin_[k].reshape(CUTS * 128, piece)).astype(BF16)
            return 0

        lax.fori_loop(0, 4, part, 0)
        spread(xs, xin, k, xsend, xrecv)

    def expert(k):
        landed(xin.at[k], xrecv.at[k])
        for b in range(4):
            y = dot(perm[...], xin[k, b * quad : (b + 1) * quad, :]).astype(BF16)
            for c in range(CUTS):
                xstk[b * unit : (b + 1) * unit, c * piece : (c + 1) * piece] = y[c * unit : (c + 1) * unit]
        gate = dot(xstk[...], wg[...])
        up = dot(xstk[...], wu[...])
        hidden = (gate / (1.0 + jnp.exp(-gate)) * up).astype(BF16)
        for c in range(CUTS):
            y = dot(hidden, wd[:, c * piece : (c + 1) * piece]).astype(BF16)
            for b in range(4):
                ystk[b, c * unit : (c + 1) * unit, :] = y[b * unit : (b + 1) * unit]
        for b in range(4):
            zs[k, b * quad : (b + 1) * quad, :] = dot(perm[...], ystk[b]).astype(BF16)
        spread(zs, zin, k, zsend, zrecv)

    def combine(k):
        landed(zin.at[k], zrecv.at[k])
        eye = jnp.where(iota((128, 128), 0) == iota((128, 128), 1), 1.0, 0.0).astype(F32)
        cols = exact_dot_nt(eye, min_[k])
        j1 = jnp.where(cols[:, 1:2] > 0.0, cols[:, 1:2] - 1.0, -1000.0)
        j2 = jnp.where(cols[:, 2:3] > 0.0, cols[:, 2:3] - 1.0, -1000.0)
        w1, w2 = cols[:, 3:4], cols[:, 4:5]
        lane = iota((128, rows), 1)
        for c in range(CUTS):
            y1 = dot(onehot(lane == j1 + float(cap * c)), zin[k])
            y2 = dot(onehot(lane == j2 + float(cap * c)), zin[k])
            rs[k, c] = (w1 * y1 + w2 * y2).astype(BF16)
        dst = rin.at[:, pl.ds(pl.multiple_of(k * 128, 128), bundle)]

        @pl.when(k == 0)
        def _():
            pltpu.make_async_copy(rs.at[0, :, pl.ds(0, bundle)], dst, rrecv.at[0]).start()

        @pl.when(k > 0)
        def _():
            pltpu.make_async_remote_copy(
                src_ref=rs.at[k, :, pl.ds(0, bundle)], dst_ref=dst, send_sem=rsend.at[k], recv_sem=rrecv.at[k],
                device_id={"ep": source(k)}, device_id_type=MESH,
            ).start()

    def stage(t, _):
        @pl.when(t < 4)
        def _():
            gather((slots - t) % slots)

        @pl.when(t == 1)
        def _():
            for c in copies:
                c.wait()

        @pl.when((t >= ET) & (t < ET + slots))
        def _():
            expert(ET + slots - 1 - t)

        @pl.when((t >= CT) & (t < CT + slots))
        def _():
            combine(CT + slots - 1 - t)

        return 0

    lax.fori_loop(0, CT + slots, stage, 0)

    for k in range(slots):
        landed(rin.at[:, pl.ds(k * 128, bundle)], rrecv.at[k])
    for c in range(CUTS):
        out_ref[:, c * piece : (c + 1) * piece] = dot(place[...], rin[c]).astype(BF16)

    for k in range(slots):
        for buf, sem in ((xs, xsend), (zs, zsend)):
            landed(buf.at[k, pl.ds(0, rows - unit)], sem.at[k])
    for k in range(1, slots):
        landed(mout.at[k], msend.at[k])
        landed(bout.at[:, pl.ds(k * 128, bundle)], bsend.at[k])
        landed(rs.at[k, :, pl.ds(0, bundle)], rsend.at[k])


def shards(n, tokens, norm_gain, route_ids, route_slots, route_weights, w_gate, w_up, w_down):
    toks, feats = tokens.shape
    hidden = w_gate.shape[2]
    top = route_ids.shape[1]
    cap = 3 * top * toks // (2 * n)
    bundle = GROUP * cap // top
    piece = feats // CUTS
    unit = CUTS * cap
    rows = GROUP * unit
    slots = 4

    vmem = pl.BlockSpec(memory_space=pltpu.VMEM)
    hbm = pl.BlockSpec(memory_space=pl.ANY)
    return pl.pallas_call(
        functools.partial(kernel, n, cap, bundle),
        out_shape=jax.ShapeDtypeStruct((toks, feats), BF16),
        in_specs=[vmem, vmem, vmem, hbm, vmem, hbm, hbm, hbm],
        out_specs=vmem,
        scratch_shapes=[
            pltpu.VMEM((toks, feats), BF16),
            pltpu.VMEM((feats, hidden), BF16),
            pltpu.VMEM((feats, hidden), BF16),
            pltpu.VMEM((hidden, feats), BF16),
            pltpu.VMEM((toks, feats), BF16),
            pltpu.VMEM((slots * 128, toks), BF16),
            pltpu.VMEM((CUTS, slots * 128, piece), BF16),
            pltpu.VMEM((slots, CUTS, 128, piece), BF16),
            pltpu.VMEM((slots, 8, 128), F32),
            pltpu.VMEM((slots, 8, 128), F32),
            pltpu.VMEM((slots, rows, piece), BF16),
            pltpu.VMEM((slots, rows, piece), BF16),
            pltpu.VMEM((slots, rows, piece), BF16),
            pltpu.VMEM((slots, rows, piece), BF16),
            pltpu.VMEM((slots, CUTS, 128, piece), BF16),
            pltpu.VMEM((CUTS, slots * 128, piece), BF16),
            pltpu.VMEM((GROUP * cap, feats), BF16),
            pltpu.VMEM((4, 4 * unit, piece), BF16),
            pltpu.VMEM((4 * unit, 4 * unit), BF16),
            pltpu.VMEM((toks, slots * 128), BF16),
            pltpu.SemaphoreType.DMA,
            pltpu.SemaphoreType.DMA((3,)),
        ] + [pltpu.SemaphoreType.DMA((slots,))] * 10,
        compiler_params=pltpu.CompilerParams(
            collective_id=0, has_side_effects=True, vmem_limit_bytes=60 * 1024 * 1024
        ),
    )(route_ids.T, route_slots.T, route_weights.T, tokens, norm_gain.reshape(1, feats), w_gate, w_up, w_down)


def solution(mesh):
    both = ("grp", "ep")
    in_specs = (
        P(both, None), P(None), P(both, None), P(both, None), P(both, None),
        P("ep", None, None), P("ep", None, None), P("ep", None, None),
    )
    return jax.shard_map(
        functools.partial(shards, mesh.shape["ep"]), mesh=mesh, in_specs=in_specs, out_specs=P(both, None),
        check_vma=False,
    )
```

```python
import functools

import jax
import jax.numpy as jnp
from jax import lax
from jax.experimental import pallas as pl
from jax.experimental.pallas import tpu as pltpu
from jax.sharding import PartitionSpec as P

MESH = pl.DeviceIdType.MESH
GROUP = 16
HALF = GROUP // 2
CUTS = 4
SENDS = (3, 2, 1)
ET, CT = 2, 5

F32 = jnp.float32
BF16 = jnp.bfloat16


def far_order(one, r):
    def pair(i, _):
        @pl.when(GROUP - 1 - i > r)
        def _():
            one(GROUP - 1 - i, 0)

        @pl.when(i < r)
        def _():
            one(i, 0)

        return 0

    lax.fori_loop(0, GROUP, pair, 0)


def onehot(mask):
    return jnp.where(mask, 1.0, 0.0).astype(BF16)


def iota(shape, dim):
    return lax.broadcasted_iota(jnp.int32, shape, dim).astype(F32)


def exact_dot_nt(a, b):
    return lax.dot_general(
        a, b, (((1,), (1,)), ((), ())), precision=lax.Precision.HIGHEST, preferred_element_type=F32
    )


def dot(a, b):
    return jnp.dot(a, b, preferred_element_type=F32)


def kernel(
    n, cap, bundle, ids_ref, spots_ref, mix_ref, tok_hbm, gain_ref, wg_hbm, wu_hbm, wd_hbm, out_ref,
    tok_ref, wg, wu, wd, nrm, pick, bout, bin_, mout, min_, xs, xin, zs, zin, rs, rin, xstk, ystk, perm, place,
    tsem, wsem, bsend, brecv, msend, mrecv, xsend, xrecv, zsend, zrecv, rsend, rrecv,
):
    toks, feats = tok_hbm.shape
    piece = feats // CUTS
    unit = CUTS * cap
    rows = GROUP * unit
    quad = 4 * unit
    slots = 4
    me = lax.axis_index("ep")
    base = (me // GROUP) * GROUP
    r = me % GROUP
    upper = (r // HALF)
    sign = 2 * upper - 1

    def wrap(dev):
        return (dev + 4 * n) % n

    def target(k):
        return wrap(me + sign * (2 * (k % 2) - 1) * HALF * k)

    def source(k):
        return wrap(me + sign * HALF * k)

    barrier = pltpu.get_barrier_semaphore()

    def greet(i, _):
        pl.semaphore_signal(barrier, inc=1, device_id={"ep": base + (r + i) % GROUP}, device_id_type=MESH)
        return 0

    lax.fori_loop(1, GROUP, greet, 0)
    for other in (wrap(me + HALF * sign), wrap(me + 3 * HALF * sign), wrap(me + 2 * HALF), wrap(me - 2 * HALF)):
        pl.semaphore_signal(barrier, inc=1, device_id={"ep": other}, device_id_type=MESH)

    tokens_in = pltpu.make_async_copy(tok_hbm, tok_ref, tsem)
    tokens_in.start()
    copies = [
        pltpu.make_async_copy(src, dst, wsem.at[i])
        for i, (src, dst) in enumerate(((wg_hbm.at[0], wg), (wu_hbm.at[0], wu), (wd_hbm.at[0], wd)))
    ]
    for c in copies:
        c.start()

    bin_[:, :, bundle:, :] = jnp.zeros_like(bin_[:, :, bundle:, :])
    for k in range(slots):
        lo = k * 128 + bundle
        rin[:, lo : lo + 128 - bundle, :] = jnp.zeros((CUTS, 128 - bundle, piece), BF16)

    step = 32
    gain = gain_ref[...]

    def norm(i, _):
        at = pl.ds(pl.multiple_of(i * step, step), step)
        x = tok_ref[at, :].astype(F32)
        scale = lax.rsqrt(jnp.mean(x * x, axis=-1, keepdims=True) + 1e-06)
        nrm[at, :] = (x * scale * gain).astype(BF16)
        return 0

    tokens_in.wait()
    lax.fori_loop(0, toks // step, norm, 0)

    ids = ids_ref[...]
    team = ids // GROUP
    rel = (team[0:1, :] - me // GROUP + slots) % slots
    near = 3 - 2 * upper
    slot_row = jnp.where(rel == 0, 0, jnp.where(rel == 2, 3, jnp.where(rel == near, 1, 2))).astype(F32)
    spots = ((ids - team * GROUP) * unit + spots_ref[...] + 1).astype(F32)
    tab = jnp.concatenate([slot_row, spots, mix_ref[...], jnp.zeros((3, toks), F32)], axis=0)
    of_slot = onehot(iota((8, toks), 0) == slot_row)
    before = onehot(iota((toks, toks), 0) < iota((toks, toks), 1))
    ranks = dot(of_slot, before)
    rank_row = jnp.sum(of_slot.astype(F32) * ranks, axis=0, keepdims=True)
    key_row = slot_row * 128.0 + rank_row
    mask = iota((slots * 128, toks), 0) == key_row
    pick[...] = onehot(mask)
    meta = exact_dot_nt(tab, jnp.where(mask, 1.0, 0.0).astype(F32))
    for k in range(slots):
        mout[k] = meta[:, k * 128 : (k + 1) * 128]
    eye = jnp.where(iota((toks, toks), 0) == iota((toks, toks), 1), 1.0, 0.0).astype(F32)
    key_col = exact_dot_nt(eye, jnp.broadcast_to(key_row, (8, toks)))[:, 0:1]
    place[...] = onehot(iota((toks, slots * 128), 1) == key_col)

    for c in range(CUTS):
        bout[c] = dot(pick[...], nrm[:, c * piece : (c + 1) * piece]).astype(BF16)

    i0 = iota((quad, quad), 0)
    a0 = jnp.floor((i0 + 0.5) / unit)
    b0 = jnp.floor((i0 - a0 * unit + 0.5) / cap)
    swapped = b0 * unit + a0 * cap + (i0 - a0 * unit - b0 * cap)
    perm[...] = onehot(iota((quad, quad), 1) == swapped)

    pl.semaphore_wait(barrier, GROUP - 1 + 4)

    def send_bundle(k):
        pltpu.make_async_remote_copy(
            src_ref=mout.at[k], dst_ref=min_.at[k], send_sem=msend.at[k], recv_sem=mrecv.at[k],
            device_id={"ep": target(k)}, device_id_type=MESH,
        ).start()
        pltpu.make_async_remote_copy(
            src_ref=bout.at[:, pl.ds(k * 128, bundle)], dst_ref=bin_.at[k, :, pl.ds(0, bundle)],
            send_sem=bsend.at[k], recv_sem=brecv.at[k],
            device_id={"ep": target(k)}, device_id_type=MESH,
        ).start()

    own_meta = pltpu.make_async_copy(mout.at[0], min_.at[0], mrecv.at[0])
    own_rows = pltpu.make_async_copy(bout.at[:, pl.ds(0, bundle)], bin_.at[0, :, pl.ds(0, bundle)], brecv.at[0])
    own_meta.start()
    own_rows.start()
    for k in SENDS:
        send_bundle(k)

    def spread(src, dst, k, send_sem, recv_sem):
        mine = pl.ds(pl.multiple_of(r * unit, 16), unit)

        def one(i, _):
            other = i
            pltpu.make_async_remote_copy(
                src_ref=src.at[k, pl.ds(pl.multiple_of(other * unit, 16), unit)], dst_ref=dst.at[k, mine],
                send_sem=send_sem.at[k], recv_sem=recv_sem.at[k],
                device_id={"ep": base + other}, device_id_type=MESH,
            ).start()
            return 0

        far_order(one, r)
        pltpu.make_async_copy(src.at[k, mine], dst.at[k, mine], recv_sem.at[k]).start()

    def landed(ref, sem):
        pltpu.make_async_copy(ref, ref, sem).wait()

    def gather(k):
        landed(min_.at[k], mrecv.at[k])
        landed(bin_.at[k, :, pl.ds(0, bundle)], brecv.at[k])
        m = min_[k]
        both = []
        for i in (1, 2):
            j = jnp.where(m[i : i + 1] > 0.0, m[i : i + 1] - 1.0, -1000.0)
            both.append(jnp.concatenate([j + float(cap * c) for c in range(CUTS)], axis=1))

        def part(b, _):
            at = pl.ds(pl.multiple_of(b * quad, quad), quad)
            row = iota((quad, CUTS * 128), 0) + (b * quad).astype(F32)
            sel = onehot((row == both[0]) | (row == both[1]))
            xs[k, at, :] = dot(sel, bin_[k].reshape(CUTS * 128, piece)).astype(BF16)
            return 0

        lax.fori_loop(0, 4, part, 0)
        spread(xs, xin, k, xsend, xrecv)

    def expert(k):
        landed(xin.at[k], xrecv.at[k])
        for b in range(4):
            y = dot(perm[...], xin[k, b * quad : (b + 1) * quad, :]).astype(BF16)
            for c in range(CUTS):
                xstk[b * unit : (b + 1) * unit, c * piece : (c + 1) * piece] = y[c * unit : (c + 1) * unit]
        gate = dot(xstk[...], wg[...])
        up = dot(xstk[...], wu[...])
        hidden = (gate / (1.0 + jnp.exp(-gate)) * up).astype(BF16)
        for c in range(CUTS):
            y = dot(hidden, wd[:, c * piece : (c + 1) * piece]).astype(BF16)
            for b in range(4):
                ystk[b, c * unit : (c + 1) * unit, :] = y[b * unit : (b + 1) * unit]
        for b in range(4):
            zs[k, b * quad : (b + 1) * quad, :] = dot(perm[...], ystk[b]).astype(BF16)
        spread(zs, zin, k, zsend, zrecv)

    def combine(k):
        landed(zin.at[k], zrecv.at[k])
        eye = jnp.where(iota((128, 128), 0) == iota((128, 128), 1), 1.0, 0.0).astype(F32)
        cols = exact_dot_nt(eye, min_[k])
        j1 = jnp.where(cols[:, 1:2] > 0.0, cols[:, 1:2] - 1.0, -1000.0)
        j2 = jnp.where(cols[:, 2:3] > 0.0, cols[:, 2:3] - 1.0, -1000.0)
        w1, w2 = cols[:, 3:4], cols[:, 4:5]
        lane = iota((128, rows), 1)
        for c in range(CUTS):
            y1 = dot(onehot(lane == j1 + float(cap * c)), zin[k])
            y2 = dot(onehot(lane == j2 + float(cap * c)), zin[k])
            rs[k, c] = (w1 * y1 + w2 * y2).astype(BF16)
        dst = rin.at[:, pl.ds(pl.multiple_of(k * 128, 128), bundle)]

        @pl.when(k == 0)
        def _():
            pltpu.make_async_copy(rs.at[0, :, pl.ds(0, bundle)], dst, rrecv.at[0]).start()

        @pl.when(k > 0)
        def _():
            pltpu.make_async_remote_copy(
                src_ref=rs.at[k, :, pl.ds(0, bundle)], dst_ref=dst, send_sem=rsend.at[k], recv_sem=rrecv.at[k],
                device_id={"ep": source(k)}, device_id_type=MESH,
            ).start()

    def stage(t, _):
        @pl.when(t < 4)
        def _():
            gather((slots - t) % slots)

        @pl.when(t == 1)
        def _():
            for c in copies:
                c.wait()

        @pl.when((t >= ET) & (t < ET + slots))
        def _():
            expert(ET + slots - 1 - t)

        @pl.when((t >= CT) & (t < CT + slots))
        def _():
            combine(CT + slots - 1 - t)

        return 0

    lax.fori_loop(0, CT + slots, stage, 0)

    for k in range(slots):
        landed(rin.at[:, pl.ds(k * 128, bundle)], rrecv.at[k])
    for c in range(CUTS):
        out_ref[:, c * piece : (c + 1) * piece] = dot(place[...], rin[c]).astype(BF16)

    for k in range(slots):
        for buf, sem in ((xs, xsend), (zs, zsend)):
            landed(buf.at[k, pl.ds(0, rows - unit)], sem.at[k])
    for k in range(1, slots):
        landed(mout.at[k], msend.at[k])
        landed(bout.at[:, pl.ds(k * 128, bundle)], bsend.at[k])
        landed(rs.at[k, :, pl.ds(0, bundle)], rsend.at[k])


def shards(n, tokens, norm_gain, route_ids, route_slots, route_weights, w_gate, w_up, w_down):
    toks, feats = tokens.shape
    hidden = w_gate.shape[2]
    top = route_ids.shape[1]
    cap = 3 * top * toks // (2 * n)
    bundle = GROUP * cap // top
    piece = feats // CUTS
    unit = CUTS * cap
    rows = GROUP * unit
    slots = 4

    vmem = pl.BlockSpec(memory_space=pltpu.VMEM)
    hbm = pl.BlockSpec(memory_space=pl.ANY)
    return pl.pallas_call(
        functools.partial(kernel, n, cap, bundle),
        out_shape=jax.ShapeDtypeStruct((toks, feats), BF16),
        in_specs=[vmem, vmem, vmem, hbm, vmem, hbm, hbm, hbm],
        out_specs=vmem,
        scratch_shapes=[
            pltpu.VMEM((toks, feats), BF16),
            pltpu.VMEM((feats, hidden), BF16),
            pltpu.VMEM((feats, hidden), BF16),
            pltpu.VMEM((hidden, feats), BF16),
            pltpu.VMEM((toks, feats), BF16),
            pltpu.VMEM((slots * 128, toks), BF16),
            pltpu.VMEM((CUTS, slots * 128, piece), BF16),
            pltpu.VMEM((slots, CUTS, 128, piece), BF16),
            pltpu.VMEM((slots, 8, 128), F32),
            pltpu.VMEM((slots, 8, 128), F32),
            pltpu.VMEM((slots, rows, piece), BF16),
            pltpu.VMEM((slots, rows, piece), BF16),
            pltpu.VMEM((slots, rows, piece), BF16),
            pltpu.VMEM((slots, rows, piece), BF16),
            pltpu.VMEM((slots, CUTS, 128, piece), BF16),
            pltpu.VMEM((CUTS, slots * 128, piece), BF16),
            pltpu.VMEM((GROUP * cap, feats), BF16),
            pltpu.VMEM((4, 4 * unit, piece), BF16),
            pltpu.VMEM((4 * unit, 4 * unit), BF16),
            pltpu.VMEM((toks, slots * 128), BF16),
            pltpu.SemaphoreType.DMA,
            pltpu.SemaphoreType.DMA((3,)),
        ] + [pltpu.SemaphoreType.DMA((slots,))] * 10,
        compiler_params=pltpu.CompilerParams(
            collective_id=0, has_side_effects=True, vmem_limit_bytes=60 * 1024 * 1024
        ),
    )(route_ids.T, route_slots.T, route_weights.T, tokens, norm_gain.reshape(1, feats), w_gate, w_up, w_down)


def solution(mesh):
    both = ("grp", "ep")
    in_specs = (
        P(both, None), P(None), P(both, None), P(both, None), P(both, None),
        P("ep", None, None), P("ep", None, None), P("ep", None, None),
    )
    return jax.shard_map(
        functools.partial(shards, mesh.shape["ep"]), mesh=mesh, in_specs=in_specs, out_specs=P(both, None),
        check_vma=False,
    )
```
